32 devices in a mesh: rep: 2 (over x), fs: 8 (over z, y), tp: 2 (over core).
Axes of the slice: x: 2, y: 2, z: 4, core: 2. Of those that a mesh axis runs over, the one named last changes fastest.
Arguments:
- tokens: bfloat16 [10240, 2048], P(('rep', 'fs'), 'tp'), may hold values from -6 to 6
- norm_first: float32 [2048], replicated, may hold values from 0.1 to 1.9
- norm_mix: float32 [2048], replicated, may hold values from 0.1 to 1.9
- norm_second: float32 [2048], replicated, may hold values from 0.1 to 1.9
- gate_weight: float32 [2048, 2816], P('fs', 'tp'), may hold values from -0.125 to 0.125
- up_weight: float32 [2048, 2816], P('fs', 'tp'), may hold values from -0.125 to 0.125
- down_weight: float32 [2816, 2048], P('tp', 'fs'), may hold values from -0.109375 to 0.109375
- gate_scale: float32 [2816], P('tp'), may hold values from 0.3 to 3
- up_scale: float32 [2816], P('tp'), may hold values from 0.3 to 3
- down_scale: float32 [2048], P('fs'), may hold values from 0.3 to 3
- u_weight: float32 [2048, 1024], P('fs', 'tp'), may hold values from -0.125 to 0.125
- v_weight: float32 [2048, 1024], P('fs', 'tp'), may hold values from -0.125 to 0.125
- u_scale: float32 [1024], P('tp'), may hold values from 0.3 to 3
- v_scale: float32 [1024], P('tp'), may hold values from 0.15 to 6
- ln_gain: float32 [1024], P('tp'), may hold values from 0.1 to 1.9
- ln_bias: float32 [1024], P('tp'), may hold values from -3 to 3
- spatial_weight: bfloat16 [8, 128, 128], P('tp'), may hold values from -0.25 to 0.25
- spatial_bias: float32 [8, 128], P('tp'), may hold values from 0.1 to 1.9
- out_weight: float32 [1024, 2048], P('tp', 'fs'), may hold values from -0.1875 to 0.1875
- out_scale: float32 [2048], P('fs'), may hold values from 0.3 to 3
Outputs:
- layer_out: bfloat16 [10240, 2048], P(('rep', 'fs'), 'tp')
The draws below stay inside these ranges and needn't reach their ends.
All inputs are finite; a program needn't handle non-finite values.
Results may differ from the reference program's by a relative error of at most 0.019.
Values may be sent and summed in bfloat16 or wider, within the bound.
No kernel may reach another device: no remote copies, remote signals or barrier semaphores. Data moves between devices by JAX's collectives and lax.ppermute only.
A program may use at most 128 MiB of HBM per device.

```python
import math
import jax
import jax.numpy as jnp
from jax import lax

D = 2048
FF = 2816
BW = 1024
SPAN = 128
GROUPS = 8
TOKENS = 10240
N_TP = 2


def draw_v_scale(key, part):
    position = jnp.arange(BW, dtype=jnp.float32) / (BW - 1)
    rough = jax.random.uniform(key, (BW,), jnp.float32, 0.6, 1.4)
    return (10.0 ** (position - 0.5) * rough).astype(jnp.float32)


def steps_of(key, shape, pieces, least, largest):
    level = 1.0
    for dim, blocks in pieces:
        draws = jax.random.uniform(jax.random.fold_in(jax.random.fold_in(key, 6), dim), (blocks,), jnp.float32, least / len(pieces), largest / len(pieces))
        level = level * jnp.repeat(jnp.exp(draws), shape[dim] // blocks).reshape((-1,) + (1,) * (len(shape) - 1 - dim))
    return level


def centred(rng, dims, deviation, limit, split=(), kind=jnp.bfloat16):
    values = deviation * jax.random.normal(rng, dims, jnp.float32)
    if split:
        values = values * steps_of(rng, dims, split, -0.22, 0.18)
    return jnp.clip(values, -limit, limit).astype(kind)


def setup_inputs(seed: int = 0) -> dict:
    splits = jax.random.split(jax.random.key(seed), 21)
    return {
        "tokens": centred(splits[0], (TOKENS, D), 1.0, 6.0, ((0, 16), (1, 2))),
        "norm_first": jnp.clip(1.0 + 0.18 * jax.random.normal(splits[1], (D,), jnp.float32), 0.1, 1.9),
        "norm_mix": jnp.clip(1.0 + 0.18 * jax.random.normal(splits[2], (D,), jnp.float32), 0.1, 1.9),
        "norm_second": jnp.clip(1.0 + 0.18 * jax.random.normal(splits[3], (D,), jnp.float32), 0.1, 1.9),
        "gate_weight": centred(splits[4], (D, FF), D ** -0.5, 0.125, ((0, 8), (1, 2)), jnp.float32),
        "up_weight": centred(splits[5], (D, FF), D ** -0.5, 0.125, ((0, 8), (1, 2)), jnp.float32),
        "down_weight": centred(splits[6], (FF, D), FF ** -0.5, 0.109375, ((0, 2), (1, 8)), jnp.float32),
        "gate_scale": jnp.clip(jnp.exp(math.log(3.0) - 2.3025851 * jax.random.uniform(splits[7], (FF,), jnp.float32) ** steps_of(splits[7], (FF,), ((0, 2),), -0.2, 0.2)), 0.3, 3.0),
        "up_scale": jnp.clip(jnp.exp(math.log(3.0) - 2.3025851 * jax.random.uniform(splits[8], (FF,), jnp.float32) ** steps_of(splits[8], (FF,), ((0, 2),), -0.2, 0.2)), 0.3, 3.0),
        "down_scale": jnp.clip(jnp.exp(math.log(3.0) - 2.3025851 * jax.random.uniform(splits[9], (D,), jnp.float32) ** steps_of(splits[9], (D,), ((0, 8),), -0.2, 0.2)), 0.3, 3.0),
        "u_weight": centred(splits[10], (D, BW), D ** -0.5, 0.125, ((0, 8), (1, 2)), jnp.float32),
        "v_weight": centred(splits[11], (D, BW), D ** -0.5, 0.125, ((0, 8), (1, 2)), jnp.float32),
        "u_scale": jnp.clip(jnp.exp(math.log(3.0) - 2.3025851 * jax.random.uniform(splits[12], (BW,), jnp.float32) ** steps_of(splits[12], (BW,), ((0, 2),), -0.2, 0.2)), 0.3, 3.0),
        "v_scale": draw_v_scale(jax.random.fold_in(splits[20], 71), 0),
        "ln_gain": jnp.clip(1.0 + 0.18 * jax.random.normal(splits[14], (BW,), jnp.float32), 0.1, 1.9),
        "ln_bias": centred(splits[15], (BW,), 0.5, 3.0, ((0, 2),), jnp.float32),
        "spatial_weight": centred(splits[16], (GROUPS, SPAN, SPAN), (4 * SPAN) ** -0.5, 0.25, ((0, 2),)),
        "spatial_bias": jnp.clip(1.0 + 0.18 * jax.random.normal(splits[17], (GROUPS, SPAN), jnp.float32), 0.1, 1.9),
        "out_weight": centred(splits[18], (BW, D), BW ** -0.5, 0.1875, ((0, 2), (1, 8)), jnp.float32),
        "out_scale": jnp.clip(jnp.exp(math.log(3.0) - 2.3025851 * jax.random.uniform(splits[19], (D,), jnp.float32) ** steps_of(splits[19], (D,), ((0, 8),), -0.2, 0.2)), 0.3, 3.0),
    }


EPS = 1e-06

def rms_norm(rows, gain):
    values = rows.astype(jnp.float32)
    scale = lax.rsqrt(lax.optimization_barrier(jnp.mean(values * values, axis=1, keepdims=True)) + EPS)
    return (values * scale * gain).astype(jnp.bfloat16)

def project(left, weight, scale):
    return jnp.dot(left, weight.astype(jnp.bfloat16), preferred_element_type=jnp.float32) * scale

def block_sum(left, weight, scale):
    width = left.shape[1] // N_TP
    total = jnp.zeros((left.shape[0], weight.shape[1]), jnp.float32)
    for index in range(N_TP):
        partial_term = project(left[:, index * width:(index + 1) * width], weight[index * width:(index + 1) * width], scale)
        partial_term = lax.optimization_barrier(partial_term.astype(jnp.bfloat16))
        total = total + partial_term.astype(jnp.float32)
    return total

def feed_forward(normed, gate_weight, up_weight, down_weight, gate_scale, up_scale, down_scale):
    gate = project(normed, gate_weight, gate_scale)
    up_part = project(normed, up_weight, up_scale)
    hidden = (jax.nn.silu(gate) * up_part).astype(jnp.bfloat16)
    return block_sum(hidden, down_weight, down_scale)

def reference(tokens, norm_first, norm_mix, norm_second, gate_weight, up_weight, down_weight, gate_scale, up_scale, down_scale, u_weight, v_weight, u_scale, v_scale, ln_gain, ln_bias, spatial_weight, spatial_bias, out_weight, out_scale):
    first = feed_forward(rms_norm(tokens, norm_first), gate_weight, up_weight, down_weight, gate_scale, up_scale, down_scale)
    middle = (tokens.astype(jnp.float32) + 0.5 * first).astype(jnp.bfloat16)
    mix_normed = rms_norm(middle, norm_mix)
    u_pre = project(mix_normed, u_weight, u_scale)
    v_pre = project(mix_normed, v_weight, v_scale)
    v_act = jax.nn.gelu(v_pre, approximate=True)
    v_mean = lax.optimization_barrier(jnp.mean(v_act, axis=1, keepdims=True))
    v_var = lax.optimization_barrier(jnp.mean(v_act * v_act, axis=1, keepdims=True)) - v_mean * v_mean
    v_normed = ((v_act - v_mean) * lax.rsqrt(v_var + EPS) * ln_gain + ln_bias).astype(jnp.bfloat16)
    count = tokens.shape[0]
    groups = spatial_weight.shape[0]
    blocks = v_normed.reshape(count // SPAN, SPAN, groups, BW // groups).astype(jnp.float32)
    lower = jnp.tril(jnp.ones((SPAN, SPAN), jnp.float32))
    masked = (spatial_weight.astype(jnp.float32) * lower[None]).astype(jnp.float32)
    spatial = jnp.einsum('gts,nsgc->ntgc', masked, blocks) + spatial_bias.T[None, :, :, None]
    mixed = (jax.nn.gelu(u_pre, approximate=True) * spatial.reshape(count, BW)).astype(jnp.bfloat16)
    second = (middle.astype(jnp.float32) + block_sum(mixed, out_weight, out_scale)).astype(jnp.bfloat16)
    last = feed_forward(rms_norm(second, norm_second), gate_weight, up_weight, down_weight, gate_scale, up_scale, down_scale)
    return (second.astype(jnp.float32) + 0.5 * last).astype(jnp.bfloat16)
```

```python
import jax
import jax.numpy as jnp
from jax import lax
from jax.experimental import pallas as pl
from jax.experimental.pallas import tpu as pltpu
from jax.sharding import PartitionSpec as P


EPS = 1e-06
LANES = 128
SPARE = 16
HBM = pl.BlockSpec(memory_space=pltpu.HBM)
VMEM = pl.BlockSpec(memory_space=pltpu.VMEM)
SMEM = pl.BlockSpec(memory_space=pltpu.SMEM)
BF, F32 = jnp.bfloat16, jnp.float32


def params():
    return pltpu.CompilerParams(vmem_limit_bytes=60 * 1024 * 1024)


def cost(flops, size):
    return pl.CostEstimate(flops=flops, bytes_accessed=size, transcendentals=0)


def lane(start):
    return pl.ds(pl.multiple_of(start * LANES, LANES), LANES)


def pack_pairs(left, right, places, stages):
    rows = left.shape[0]

    def body(at, l_ref, r_ref, *outs):
        outs = iter(outs)
        for stage in stages:
            for group in (stage.near, stage.far_z):
                out = next(outs)
                for k, place in enumerate(group):
                    n = at[place]
                    out[0, :, 2 * k * LANES : (2 * k + 1) * LANES] = l_ref[:, lane(n)].astype(BF)
                    out[0, :, (2 * k + 1) * LANES : (2 * k + 2) * LANES] = r_ref[:, lane(n)].astype(BF)

    shapes = [
        jax.ShapeDtypeStruct((1, rows, 2 * LANES * len(group)), BF) for stage in stages for group in (stage.near, stage.far_z)
    ]
    out = pl.pallas_call(
        body,
        out_shape=shapes,
        in_specs=[SMEM, VMEM, VMEM],
        out_specs=[VMEM] * len(shapes),
        compiler_params=params(),
        cost_estimate=cost(1000, 6 * left.size * 2),
    )(places, left, right)
    return [(out[2 * i], out[2 * i + 1]) for i in range(len(stages))]


def pack_rows(weight, scale, places, stage):
    columns = weight.shape[1]

    def body(at, w_ref, s_ref, near_ref, far_ref):
        for k, place in enumerate(stage.near):
            near_ref[0, SPARE + k * LANES : SPARE + (k + 1) * LANES, :] = w_ref[lane(at[place]), :].astype(BF)
        for k, place in enumerate(stage.far_z):
            far_ref[0, k * LANES : (k + 1) * LANES, :] = w_ref[lane(at[place]), :].astype(BF)
        value = s_ref[...]
        high = value.astype(BF)
        rest = value - high.astype(F32)
        mid = rest.astype(BF)
        low = (rest - mid.astype(F32)).astype(BF)
        row = lax.broadcasted_iota(jnp.int32, (SPARE, columns), 0)
        pick = jnp.where(row == 0, high.astype(F32), jnp.where(row == 1, mid.astype(F32), jnp.where(row == 2, low.astype(F32), 0.0)))
        near_ref[0, :SPARE, :] = pick.astype(BF)

    return pl.pallas_call(
        body,
        out_shape=[
            jax.ShapeDtypeStruct((1, len(stage.near) * LANES + SPARE, columns), BF),
            jax.ShapeDtypeStruct((1, len(stage.far_z) * LANES, columns), BF),
        ],
        in_specs=[SMEM, VMEM, VMEM],
        out_specs=[VMEM, VMEM],
        compiler_params=params(),
        cost_estimate=cost(1000, 6 * weight.size),
    )(places, weight, scale.reshape(1, columns))


class Stage:
    def __init__(self, name, tiles, unit, axis, head):
        self.name, self.tiles, self.unit, self.axis, self.head = name, tiles, unit, axis, head
        n = len(tiles)
        self.fz, self.fy = max(1, n // 5), n // 2
        back = list(reversed(tiles))
        self.near, self.far_z = tiles[: n - self.fz], back[: self.fz]
        self.near_y, self.far_y = tiles[: n - self.fy], back[: self.fy]

    def runs(self):
        out = []
        unit, head, fz, fy = self.unit, self.head, self.fz, self.fy

        def put(piece, block, count, offset, tiles, with_head=False):
            at = offset
            if with_head:
                at += head
            k = 0
            while k < len(tiles):
                n = 1
                while k + n < len(tiles) and tiles[k + n] == tiles[k] + n:
                    n += 1
                start, size, place = at + k * unit, n * unit, head + tiles[k] * unit
                if with_head and head and k == 0:
                    if tiles[0] == 0:
                        start, size, place = start - head, size + head, place - head
                    else:
                        out.append((piece, block, count, offset, 0, head))
                out.append((piece, block, count, start, place, size))
                k += n

        put(0, 0, 1, 0, self.near, True)
        put(1, 1, 1, 0, self.near, True)
        put(2, 2, 2, 0, self.near, True)
        put(3, 0, 1, 0, self.far_z)
        put(4, 4, 2, 0, self.near_y, True)
        put(5, 6, 2, 0, self.near_y, True)
        put(6, 1, 1, 0, self.far_z)
        put(6, 4, 1, fz * unit, self.far_y)
        put(6, 5, 1, (fz + fy) * unit, self.far_y)
        put(7, 2, 2, 0, self.far_z)
        put(7, 6, 2, fz * unit, self.far_y)
        return out


N_PIECES = 8


def fetches(stage, pieces, scratch, sems, first):
    out = []
    for piece, block, count, start, place, size in stage.runs():
        if stage.axis == 2:
            source = pieces[piece].at[:, :, pl.ds(start, size)]
            target = scratch.at[pl.ds(block, count), :, pl.ds(place, size)]
        else:
            source = pieces[piece].at[:, pl.ds(start, size), :]
            target = scratch.at[pl.ds(block, count), pl.ds(place, size), :]
        out.append(pltpu.make_async_copy(source, target, sems.at[first + len(out)]))
    return out


def norm_rows(rows, gains):
    values = rows.astype(F32)
    factor = lax.rsqrt(jnp.mean(values * values, axis=1, keepdims=True) + EPS)
    return (values * factor * gains).astype(BF)


def local_gain(gain_ref, at, blocks):
    return jnp.concatenate([gain_ref[pl.ds(at[l], 1), :] for l in range(blocks)], axis=1)


def residual_and_norm(rest, weight, terms, gains, new_ref, normed, step):
    count, _ = rest.shape

    @pl.loop(0, count // step, unroll=4)
    def _(i):
        here = pl.ds(pl.multiple_of(i * step, step), step)
        rows = rest[here, :]
        if terms:
            total = terms[0][here, :].astype(F32) + terms[1][here, :].astype(F32)
            rows = (rows.astype(F32) + weight * total).astype(BF)
            new_ref[here, :] = rows
        normed[here, :] = norm_rows(rows, gains)


def flat(ref, columns):
    block = ref[:, :, columns]
    return block.reshape(block.shape[0] * block.shape[1], block.shape[2])


def hidden_units(config, place, normed, w_up, gs_ref, us_ref, out):
    tiles, chunk = config["tiles"], config["chunk"]

    @pl.loop(0, normed.shape[0] // chunk)
    def _(i):
        here = pl.ds(pl.multiple_of(i * chunk, chunk), chunk)
        lhs = normed[here, :]
        for k in range(tiles):
            rhs = flat(w_up, slice(2 * k * LANES, (2 * k + 2) * LANES))
            acc = jnp.dot(lhs, rhs, preferred_element_type=F32)
            n = place[k]
            gate = acc[:, :LANES] * gs_ref[pl.ds(n, 1), :]
            up_part = acc[:, LANES:] * us_ref[pl.ds(n, 1), :]
            out[here, k * LANES : (k + 1) * LANES] = (gate / (1.0 + jnp.exp(-gate)) * up_part).astype(BF)


def feed_forward(config, ids, state, gain, stages, pieces, scales, last):
    blocks, tiles, chunk, place_of = config["blocks"], config["tiles"], config["chunk"], config["place"]
    count, width = state[0].shape
    columns = width // blocks
    units = tiles * LANES
    n_state = len(state)
    n_copies = sum(len(stage.runs()) for stage in stages)

    def body(*refs):
        at, place, refs = refs[0], refs[1], refs[2:]
        sources, refs = refs[:n_state], refs[n_state:]
        gain_ref, gs_ref, us_ref, refs = refs[0], refs[1], refs[2], refs[3:]
        parts = [refs[N_PIECES * i : N_PIECES * (i + 1)] for i in range(len(stages))]
        refs = refs[N_PIECES * len(stages) :]
        n_out = 3 if last else len(state[:2])
        outs, refs = refs[:n_out], refs[n_out:]
        w_up, w_down, normed, hidden, sems, refs = refs[0], refs[1], refs[2], refs[3], refs[4], refs[5:]
        st, refs = refs[:n_state], refs[n_state:]
        loads = [pltpu.make_async_copy(a, b, sems.at[n_copies + k]) for k, (a, b) in enumerate(zip(sources, st))]
        up = fetches(stages[0], parts[0], w_up, sems, 0)
        up += fetches(stages[1], parts[1], w_up, sems, len(up))
        down = fetches(stages[2], parts[2], w_down, sems, len(up))
        for copy in loads + up + down:
            copy.start()
        gains = local_gain(gain_ref, at, blocks)
        for copy in loads:
            copy.wait()
        residual_and_norm(st[0], 0.5 if not last else 1.0, st[1:], gains, st[0], normed, 16)
        saves = []
        if n_state > 1 and not last:
            saves.append(pltpu.make_async_copy(st[0], outs[1], sems.at[n_copies + 3]))
            saves[0].start()
        for copy in up:
            copy.wait()

        hidden_units(config, place, normed, w_up, gs_ref, us_ref, hidden)

        for copy in down:
            copy.wait()
        halves, rests = refs if last else (refs[0], None)

        @pl.loop(0, count // chunk)
        def _(i):
            here = pl.ds(pl.multiple_of(i * chunk, chunk), chunk)
            left = hidden[here, :]
            for l in range(blocks):
                acc = jnp.dot(left, w_down[l, SPARE:, :], preferred_element_type=F32)
                terms = w_down[l, :SPARE, :].astype(F32)
                value = (acc * (terms[0:1] + terms[1:2] + terms[2:3])).astype(BF)
                block = slice(l * columns, (l + 1) * columns)
                if not last:
                    halves[here, block] = value
                else:
                    j = at[l]
                    side = jnp.where(lax.div(j, blocks // 2) == at[blocks], 0, 1)
                    there = pl.ds(pl.multiple_of(lax.rem(j, blocks // 2) * columns, columns), columns)
                    halves[side, here, there] = value
                    rests[side, here, there] = st[0][here, block]

        if last:
            results = ((halves.at[1], outs[1]), (halves.at[0], outs[0]), (rests.at[0], outs[2]))
        else:
            results = ((halves, outs[0]),)
        results = [pltpu.make_async_copy(a, b, sems.at[n_copies + 4 + k]) for k, (a, b) in enumerate(results)]
        for copy in results:
            copy.start()
        for copy in results + saves:
            copy.wait()

    if last:
        shapes = [jax.ShapeDtypeStruct((count, width // 2), BF)] * 3
        extra = [pltpu.VMEM((2, count, width // 2), BF)] * 2
    else:
        shapes = [jax.ShapeDtypeStruct((count, width), BF)] * len(state[:2])
        extra = [pltpu.VMEM((count, width), BF)]
    return pl.pallas_call(
        body,
        out_shape=shapes,
        in_specs=[SMEM, SMEM] + [HBM] * n_state + [VMEM] * 3 + [HBM] * (N_PIECES * len(stages)),
        out_specs=[HBM] * len(shapes),
        scratch_shapes=[
            pltpu.VMEM((blocks, columns, 2 * units), BF),
            pltpu.VMEM((blocks, SPARE + units, columns), BF),
            pltpu.VMEM((count, width), BF),
            pltpu.VMEM((count, units), BF),
            pltpu.SemaphoreType.DMA((n_copies + 8,)),
        ]
        + [pltpu.VMEM((count, width), BF)] * n_state
        + extra,
        compiler_params=params(),
        cost_estimate=cost(6 * count * width * units, 2 * 3 * width * units),
    )(
        ids,
        place_of,
        *state,
        gain.reshape(blocks, columns),
        scales[0].reshape(tiles, LANES),
        scales[1].reshape(tiles, LANES),
        *[p for group in pieces for p in group],
    )


def first_hidden(config, ids, state, gain, stages, pieces, scales):
    blocks, tiles = config["blocks"], config["tiles"]
    count, width = state.shape
    columns, units = width // blocks, tiles * LANES
    n_copies = sum(len(stage.runs()) for stage in stages)

    def body(at, place, source, gain_ref, gs_ref, us_ref, *refs):
        parts = [refs[N_PIECES * i : N_PIECES * (i + 1)] for i in range(len(stages))]
        out, w_up, normed, sems, st = refs[N_PIECES * len(stages) :]
        load = pltpu.make_async_copy(source, st, sems.at[n_copies])
        up = []
        for stage, part in zip(stages, parts):
            up += fetches(stage, part, w_up, sems, len(up))
        for copy in [load] + up:
            copy.start()
        gains = local_gain(gain_ref, at, blocks)
        load.wait()
        residual_and_norm(st, 0.5, (), gains, None, normed, 16)
        for copy in up:
            copy.wait()
        hidden_units(config, place, normed, w_up, gs_ref, us_ref, out)

    return pl.pallas_call(
        body,
        out_shape=jax.ShapeDtypeStruct((count, units), BF),
        in_specs=[SMEM, SMEM, HBM] + [VMEM] * 3 + [HBM] * (N_PIECES * len(stages)),
        out_specs=VMEM,
        scratch_shapes=[
            pltpu.VMEM((blocks, columns, 2 * units), BF),
            pltpu.VMEM((count, width), BF),
            pltpu.SemaphoreType.DMA((n_copies + 1,)),
            pltpu.VMEM((count, width), BF),
        ],
        compiler_params=params(),
        cost_estimate=cost(4 * count * width * units, 2 * 2 * width * units),
    )(
        ids,
        config["place"],
        state,
        gain.reshape(blocks, columns),
        scales[0].reshape(tiles, LANES),
        scales[1].reshape(tiles, LANES),
        *[p for group in pieces for p in group],
    )


def first_down(config, hidden, stage, pieces):
    blocks, chunk, width = config["blocks"], config["chunk"], config["width"]
    count, units = hidden.shape
    columns = width // blocks
    n_copies = len(stage.runs())

    def body(left_ref, *refs):
        out, w_down, sems = refs[N_PIECES:]
        copies = fetches(stage, refs[:N_PIECES], w_down, sems, 0)
        for copy in copies:
            copy.start()
        for copy in copies:
            copy.wait()

        @pl.loop(0, count // chunk)
        def _(i):
            here = pl.ds(pl.multiple_of(i * chunk, chunk), chunk)
            left = left_ref[here, :]
            for l in range(blocks):
                acc = jnp.dot(left, w_down[l, SPARE:, :], preferred_element_type=F32)
                terms = w_down[l, :SPARE, :].astype(F32)
                out[here, l * columns : (l + 1) * columns] = (acc * (terms[0:1] + terms[1:2] + terms[2:3])).astype(BF)

    return pl.pallas_call(
        body,
        out_shape=jax.ShapeDtypeStruct((count, width), BF),
        in_specs=[VMEM] + [HBM] * N_PIECES,
        out_specs=VMEM,
        scratch_shapes=[pltpu.VMEM((blocks, SPARE + units, columns), BF), pltpu.SemaphoreType.DMA((n_copies,))],
        compiler_params=params(),
        cost_estimate=cost(2 * count * width * units, 2 * width * units),
    )(hidden, *pieces)


def gelu(a):
    return 0.5 * a * (1.0 + jnp.tanh(0.7978845608028654 * (a + 0.044715 * a * a * a)))


def mixer_in(config, ids, state, gain, stage, pieces, scales):
    blocks, tiles, chunk = config["blocks"], config["tiles"], config["chunk"]
    count, width = state[0].shape
    columns = width // blocks
    n_copies = len(stage.runs())

    def body(*refs):
        at, place, refs = refs[0], refs[1], refs[2:]
        sources, gain_ref, us_ref, vs_ref = refs[:3], refs[3], refs[4], refs[5]
        parts, refs = refs[6 : 6 + N_PIECES], refs[6 + N_PIECES :]
        new_out, u_out, v_out, sum_out, w, normed, sems, *st = refs
        loads = [pltpu.make_async_copy(a, b, sems.at[n_copies + k]) for k, (a, b) in enumerate(zip(sources, st))]
        copies = fetches(stage, parts, w, sems, 0)
        for copy in loads + copies:
            copy.start()
        gains = local_gain(gain_ref, at, blocks)
        for copy in loads:
            copy.wait()
        residual_and_norm(st[0], 0.5, st[1:], gains, st[0], normed, 16)
        save = pltpu.make_async_copy(st[0], new_out, sems.at[n_copies + 3])
        save.start()
        for copy in copies:
            copy.wait()

        @pl.loop(0, count // chunk)
        def _(i):
            here = pl.ds(pl.multiple_of(i * chunk, chunk), chunk)
            lhs = normed[here, :]
            plain = jnp.zeros((chunk, LANES), F32)
            square = jnp.zeros((chunk, LANES), F32)
            for k in range(tiles):
                rhs = flat(w, slice(2 * k * LANES, (2 * k + 2) * LANES))
                acc = jnp.dot(lhs, rhs, preferred_element_type=F32)
                n = place[k]
                block = slice(k * LANES, (k + 1) * LANES)
                u_out[here, block] = gelu(acc[:, :LANES] * us_ref[pl.ds(n, 1), :])
                v_act = gelu(acc[:, LANES:] * vs_ref[pl.ds(n, 1), :])
                v_out[here, block] = v_act
                plain += v_act
                square += v_act * v_act
            index = lax.broadcasted_iota(jnp.int32, (chunk, LANES), 1)
            sum_out[here, :] = jnp.where(
                index == 0, jnp.sum(plain, axis=1, keepdims=True), jnp.sum(square, axis=1, keepdims=True)
            )

        save.wait()

    return pl.pallas_call(
        body,
        out_shape=[
            jax.ShapeDtypeStruct((count, width), BF),
            jax.ShapeDtypeStruct((count, tiles * LANES), F32),
            jax.ShapeDtypeStruct((count, tiles * LANES), F32),
            jax.ShapeDtypeStruct((count, LANES), F32),
        ],
        in_specs=[SMEM, SMEM] + [HBM] * 3 + [VMEM] * 3 + [HBM] * N_PIECES,
        out_specs=[HBM] + [VMEM] * 3,
        scratch_shapes=[
            pltpu.VMEM((blocks, columns, 2 * tiles * LANES), BF),
            pltpu.VMEM((count, width), BF),
            pltpu.SemaphoreType.DMA((n_copies + 4,)),
        ]
        + [pltpu.VMEM((count, width), BF)] * 3,
        compiler_params=params(),
        cost_estimate=cost(4 * count * width * tiles * LANES, 4 * width * tiles * LANES),
    )(
        ids,
        config["place"],
        *state,
        gain.reshape(blocks, columns),
        scales[0].reshape(tiles, LANES),
        scales[1].reshape(tiles, LANES),
        *pieces,
    )


def mixer_out(config, u_act, v_act, sums, other, layer, spatial_weight, spatial_bias, stage, pieces):
    blocks, tiles, chunk, width = config["blocks"], config["tiles"], config["chunk"], config["width"]
    count, channels = u_act.shape
    columns = width // blocks
    span = spatial_weight.shape[1]
    n_copies = len(stage.runs())
    share = 0.5 / channels

    def body(*refs):
        place, u_ref, v_ref, s_ref, o_ref, gain_ref, bias_ref, w_ref, b_ref = refs[:9]
        parts, refs = refs[9 : 9 + N_PIECES], refs[9 + N_PIECES :]
        out, w_out, mixed, sems = refs
        copies = fetches(stage, parts, w_out, sems, 0)
        for copy in copies:
            copy.start()
        total = s_ref[...] + o_ref[...]
        mean = total[:, 0:1] * share
        var = total[:, 1:2] * share - mean * mean
        factor = lax.rsqrt(var + EPS)
        keep = lax.broadcasted_iota(jnp.int32, (span, span), 0) >= lax.broadcasted_iota(jnp.int32, (span, span), 1)
        for t in range(tiles):
            n = place[t]
            block = slice(t * LANES, (t + 1) * LANES)
            v_normed = ((v_ref[:, block] - mean) * factor * gain_ref[pl.ds(n, 1), :] + bias_ref[pl.ds(n, 1), :]).astype(BF)
            side = jnp.concatenate([v_normed[m * span : (m + 1) * span] for m in range(count // span)], axis=1)
            w = jnp.where(keep, w_ref[n].astype(F32), 0.0).astype(BF)
            turned = jnp.dot(w, side, preferred_element_type=F32)
            shift = b_ref[n]
            for m in range(count // span):
                here = slice(m * span, (m + 1) * span)
                spatial = turned[:, m * LANES : (m + 1) * LANES] + shift
                mixed[here, block] = (u_ref[here, block] * spatial).astype(BF)
        for copy in copies:
            copy.wait()

        @pl.loop(0, count // chunk)
        def _(i):
            here = pl.ds(pl.multiple_of(i * chunk, chunk), chunk)
            left = mixed[here, :]
            for l in range(blocks):
                acc = jnp.dot(left, w_out[l, SPARE:, :], preferred_element_type=F32)
                terms = w_out[l, :SPARE, :].astype(F32)
                out[here, l * columns : (l + 1) * columns] = (acc * (terms[0:1] + terms[1:2] + terms[2:3])).astype(BF)

    return pl.pallas_call(
        body,
        out_shape=jax.ShapeDtypeStruct((count, width), BF),
        in_specs=[SMEM] + [VMEM] * 8 + [HBM] * N_PIECES,
        out_specs=VMEM,
        scratch_shapes=[
            pltpu.VMEM((blocks, SPARE + channels, columns), BF),
            pltpu.VMEM((count, channels), BF),
            pltpu.SemaphoreType.DMA((n_copies,)),
        ],
        compiler_params=params(),
        cost_estimate=cost(2 * count * width * channels, 2 * width * channels),
    )(
        config["place"],
        u_act,
        v_act,
        sums,
        other,
        layer[0].reshape(tiles, LANES),
        layer[1].reshape(tiles, LANES),
        spatial_weight,
        jnp.broadcast_to(spatial_bias[:, :, None], (tiles, span, LANES)),
        *pieces,
    )


SWAP = [(0, 1), (1, 0)]
NZ, NY = 4, 2


def join(body, shapes, flag, *values):
    return pl.pallas_call(
        body,
        out_shape=[jax.ShapeDtypeStruct(shape, BF) for shape in shapes],
        in_specs=[SMEM] + [VMEM] * len(values),
        out_specs=[VMEM] * len(shapes),
        compiler_params=params(),
        cost_estimate=cost(1000000, 4 * sum(v.size for v in values)),
    )(flag, *values)


def gather(stage, near, far, outer):
    at = lambda z, y: z * NY + y
    pairs = lambda hops: [(at(a, y), at(b, y)) for a, b in hops for y in range(NY)]
    across = [(at(z, y), at(z, 1 - y)) for z in range(NZ) for y in range(NY)]
    axis = stage.axis
    unit, head = stage.unit, stage.head
    all_z, all_y = head + len(stage.near) * unit, head + len(stage.near_y) * unit
    fz, fy = stage.fz * unit, stage.fy * unit

    def shape(blocks, size):
        out = [blocks, near.shape[1], near.shape[2]]
        out[axis] = size
        return tuple(out)

    def part(ref, block, start, size):
        return ref.at[block, pl.ds(start, size), :] if axis == 1 else ref.at[block, :, pl.ds(start, size)]

    def put(to, block, start, source, at, begin, size):
        part(to, block, start, size)[...] = part(source, at, begin, size)[...]

    def join_e(_, near_ref, e_ref, m_ref, y_ref):
        for k, ref in enumerate((near_ref, e_ref)):
            put(m_ref, k, 0, ref, 0, 0, all_z)
            put(y_ref, k, 0, ref, 0, 0, all_y)

    def join_p(_, e_ref, y_ref, p_ref):
        put(p_ref, 0, 0, e_ref, 0, head, fz)
        for k in range(2):
            put(p_ref, 0, fz + k * fy, y_ref, k, head, fy)

    def join_g(is_outer, g_ref, m_ref, two_ref, r_ref):
        def take(ref):
            for k in range(2):
                put(two_ref, k, 0, ref, k, 0, all_z)
                put(r_ref, k, 0, ref, k, 0, all_y)

        pl.when(is_outer[0] == 1)(lambda: take(g_ref))
        pl.when(is_outer[0] == 0)(lambda: take(m_ref))

    def join_q(_, two_ref, r_ref, q_ref):
        for k in range(2):
            put(q_ref, k, 0, two_ref, k, head, fz)
            put(q_ref, k, fz, r_ref, k, head, fy)

    e = lax.ppermute(near, "fs", pairs([(0, 1), (1, 0), (2, 3), (3, 2)]))
    m, y = join(join_e, [shape(2, all_z), shape(2, all_y)], outer, near, e)
    m = lax.ppermute(m, "fs", pairs([(1, 2), (2, 1)]))
    y = lax.ppermute(y, "fs", across)
    g = lax.ppermute(m, "fs", pairs([(1, 0), (2, 3)]))
    (p,) = join(join_p, [shape(1, fz + 2 * fy)], outer, e, y)
    p = lax.ppermute(p, "rep", SWAP)
    two, r = join(join_g, [shape(2, all_z), shape(2, all_y)], outer, g, m)
    r = lax.ppermute(r, "fs", across)
    (q,) = join(join_q, [shape(2, fz + fy)], outer, two, r)
    q = lax.ppermute(q, "rep", SWAP)
    return [near, e, two, far, y, r, p, q]


def fast(*args):
    (tokens, norm_first, norm_mix, norm_second, gate_weight, up_weight, down_weight, gate_scale, up_scale, down_scale,
     u_weight, v_weight, u_scale, v_scale, ln_gain, ln_bias, spatial_weight, spatial_bias, out_weight, out_scale) = args
    count, half = tokens.shape
    width = 2 * half
    blocks = NZ * NY
    columns = width // blocks
    rep, tp, fs = lax.axis_index("rep"), lax.axis_index("tp"), lax.axis_index("fs")
    z, y = fs // NY, fs % NY
    outer = jnp.logical_or(z == 0, z == NZ - 1).astype(jnp.int32).reshape(1)
    low = z < 2
    layers = (z, z + 1 - 2 * (z % 2), jnp.where(low, 2, 1), jnp.where(low, 3, 0))
    ids = jnp.stack([layer * NY + row for row in (y, 1 - y) for layer in layers] + [tp]).astype(jnp.int32)
    ff_tiles, bw_tiles = gate_weight.shape[1] // LANES, u_weight.shape[1] // LANES

    def places(tiles):
        index = jnp.arange(tiles, dtype=jnp.int32)
        return jnp.where(rep == 0, index, tiles - 1 - index)

    ff_place, bw_place = places(ff_tiles), places(bw_tiles)
    rim = ff_tiles // 5
    every = list(range(ff_tiles))
    outside = every[:rim] + [ff_tiles // 2] * (ff_tiles % 2) + every[ff_tiles - rim :]
    inside = [k for k in every if k not in outside]
    g1, g2 = Stage("g1", outside, 2 * LANES, 2, 0), Stage("g2", inside, 2 * LANES, 2, 0)
    dn = Stage("dn", every, LANES, 1, SPARE)
    uv = Stage("uv", list(range(bw_tiles)), 2 * LANES, 2, 0)
    ou = Stage("ou", list(range(bw_tiles)), LANES, 1, SPARE)
    own = {}
    own["g1"], own["g2"] = pack_pairs(gate_weight, up_weight, ff_place, [g1, g2])
    own["dn"] = pack_rows(down_weight, down_scale, ff_place, dn)
    (own["uv"],) = pack_pairs(u_weight, v_weight, bw_place, [uv])
    own["ou"] = pack_rows(out_weight, out_scale, bw_place, ou)
    peer = lax.ppermute(tokens, "tp", SWAP)
    pieces = {s.name: gather(s, *own[s.name], outer) for s in (g1, g2, dn, uv, ou)}
    full = jnp.where(tp == 0, jnp.concatenate([tokens, peer], axis=1), jnp.concatenate([peer, tokens], axis=1))
    start = jnp.concatenate([lax.dynamic_slice_in_dim(full, ids[l] * columns, columns, axis=1) for l in range(blocks)], axis=1)
    chunk = count // 2
    ff = {"blocks": blocks, "tiles": ff_tiles, "chunk": chunk, "place": ff_place, "width": width}
    mix = {"blocks": blocks, "tiles": bw_tiles, "chunk": chunk, "place": bw_place, "width": width}
    ff_stages, ff_pieces = (g1, g2, dn), [pieces["g1"], pieces["g2"], pieces["dn"]]
    hidden = first_hidden(ff, ids, start, norm_first, ff_stages[:2], ff_pieces[:2], (gate_scale, up_scale))
    first = first_down(ff, hidden, dn, pieces["dn"])
    first_in = lax.ppermute(first, "tp", SWAP)
    middle, u_act, v_act, sums = mixer_in(mix, ids, (start, first, first_in), norm_mix, uv, pieces["uv"], (u_scale, v_scale))
    sums_in = lax.ppermute(sums, "tp", SWAP)
    mixed = mixer_out(mix, u_act, v_act, sums, sums_in, (ln_gain, ln_bias), spatial_weight, spatial_bias, ou, pieces["ou"])
    mixed_in = lax.ppermute(mixed, "tp", SWAP)
    own_last, send, rest = feed_forward(
        ff, ids, (middle, mixed, mixed_in), norm_second, ff_stages, ff_pieces, (gate_scale, up_scale), True)
    got = lax.ppermute(send, "tp", SWAP)
    return (rest.astype(F32) + 0.5 * (own_last.astype(F32) + got.astype(F32))).astype(BF)


def plain(*args):
    (tokens, norm_first, norm_mix, norm_second, gate_weight, up_weight, down_weight, gate_scale, up_scale, down_scale,
     u_weight, v_weight, u_scale, v_scale, ln_gain, ln_bias, spatial_weight, spatial_bias, out_weight, out_scale) = args
    gather = lambda v, axis: lax.all_gather(v, "fs", axis=axis, tiled=True)
    count, n_tp = tokens.shape[0], lax.axis_size("tp")
    span = spatial_weight.shape[1]

    def full_norm(rows, gain):
        values = lax.all_gather(rows, "tp", axis=1, tiled=True).astype(F32)
        factor = lax.rsqrt(jnp.mean(values * values, axis=1, keepdims=True) + EPS)
        return (values * factor * gain).astype(BF)

    def spread_sum(term):
        return lax.psum_scatter(term.astype(BF), "tp", scatter_dimension=1, tiled=True).astype(F32)

    def dot(left, right):
        return jnp.dot(left, right, preferred_element_type=F32)

    gate_all, up_all, down_all = gather(gate_weight.astype(BF), 0), gather(up_weight.astype(BF), 0), gather(down_weight.astype(BF), 1)
    down_scales, out_scales = gather(down_scale, 0), gather(out_scale, 0)

    def feed(rows, gain):
        normed = full_norm(rows, gain)
        hidden = (jax.nn.silu(dot(normed, gate_all) * gate_scale) * (dot(normed, up_all) * up_scale)).astype(BF)
        return spread_sum(dot(hidden, down_all) * down_scales)

    middle = (tokens.astype(F32) + 0.5 * feed(tokens, norm_first)).astype(BF)
    normed = full_norm(middle, norm_mix)
    u_pre = dot(normed, gather(u_weight.astype(BF), 0)) * u_scale
    v_act = gelu(dot(normed, gather(v_weight.astype(BF), 0)) * v_scale)
    sums = lax.psum((jnp.sum(v_act, axis=1), jnp.sum(v_act * v_act, axis=1)), "tp")
    channels = v_act.shape[1]
    v_mean = (sums[0] / (n_tp * channels))[:, None]
    v_var = (sums[1] / (n_tp * channels))[:, None] - v_mean * v_mean
    v_normed = ((v_act - v_mean) * lax.rsqrt(v_var + EPS) * ln_gain + ln_bias).astype(BF)
    groups = spatial_weight.shape[0]
    tiles = v_normed.reshape(count // span, span, groups, channels // groups)
    lower = jnp.tril(jnp.ones((span, span), jnp.bool_))
    masked = jnp.where(lower[None], spatial_weight, jnp.zeros_like(spatial_weight))
    spatial = jnp.einsum("gts,nsgc->ntgc", masked, tiles, preferred_element_type=F32) + spatial_bias.T[None, :, :, None]
    mixed = (gelu(u_pre) * spatial.reshape(count, channels)).astype(BF)
    second = (middle.astype(F32) + spread_sum(dot(mixed, gather(out_weight.astype(BF), 1)) * out_scales)).astype(BF)
    return (second.astype(F32) + 0.5 * feed(second, norm_second)).astype(BF)


def solution(mesh):
    tokens = P(("rep", "fs"), "tp")
    rows, columns = P("fs", "tp"), P("tp", "fs")
    tp, fs, whole = P("tp"), P("fs"), P()
    placed = (
        tokens, whole, whole, whole, rows, rows, columns, tp, tp, fs, rows, rows, tp, tp, tp, tp,
        P("tp", None, None), P("tp", None), columns, fs,
    )

    def on_device(*args):
        block = args[4].shape[0]
        tidy = block % (2 * LANES) == 0 and args[4].shape[1] % LANES == 0 and args[10].shape[1] % LANES == 0
        if tidy and mesh.shape["fs"] == NZ * NY and mesh.shape["rep"] == 2 and mesh.shape["tp"] == 2:
            return fast(*args)
        return plain(*args)

    return jax.shard_map(on_device, mesh=mesh, in_specs=placed, out_specs=tokens, check_vma=False)
```

```python
import jax
import jax.numpy as jnp
from jax import lax
from jax.experimental import pallas as pl
from jax.experimental.pallas import tpu as pltpu
from jax.sharding import PartitionSpec as P


EPS = 1e-06
LANES = 128
SPARE = 16
HBM = pl.BlockSpec(memory_space=pltpu.HBM)
ANY = pl.BlockSpec(memory_space=pl.ANY)
VMEM = pl.BlockSpec(memory_space=pltpu.VMEM)
SMEM = pl.BlockSpec(memory_space=pltpu.SMEM)
BF, F32 = jnp.bfloat16, jnp.float32


def params(mebibytes):
    return pltpu.CompilerParams(vmem_limit_bytes=mebibytes * 1024 * 1024)


def cost(flops, size):
    return pl.CostEstimate(flops=flops, bytes_accessed=size, transcendentals=0)


def lane(start):
    return pl.ds(pl.multiple_of(start * LANES, LANES), LANES)


def pack_pairs(left, right, places, stages):
    rows = left.shape[0]

    def body(at, l_ref, r_ref, *outs):
        outs = iter(outs)
        for stage in stages:
            for group in (stage.near, stage.far_z):
                out = next(outs)
                for k, place in enumerate(group):
                    n = at[place]
                    out[0, :, 2 * k * LANES : (2 * k + 1) * LANES] = l_ref[:, lane(n)].astype(BF)
                    out[0, :, (2 * k + 1) * LANES : (2 * k + 2) * LANES] = r_ref[:, lane(n)].astype(BF)

    shapes = [
        jax.ShapeDtypeStruct((1, rows, 2 * LANES * len(group)), BF) for stage in stages for group in (stage.near, stage.far_z)
    ]
    out = pl.pallas_call(
        body,
        out_shape=shapes,
        in_specs=[SMEM, VMEM, VMEM],
        out_specs=[VMEM] * len(shapes),
        compiler_params=params(16),
        cost_estimate=cost(1000, 6 * left.size * 2),
    )(places, left, right)
    return [(out[2 * i], out[2 * i + 1]) for i in range(len(stages))]


def pack_rows(weight, scale, places, stage):
    columns = weight.shape[1]

    def body(at, w_ref, s_ref, near_ref, far_ref):
        for k, place in enumerate(stage.near):
            near_ref[0, SPARE + k * LANES : SPARE + (k + 1) * LANES, :] = w_ref[lane(at[place]), :].astype(BF)
        for k, place in enumerate(stage.far_z):
            far_ref[0, k * LANES : (k + 1) * LANES, :] = w_ref[lane(at[place]), :].astype(BF)
        value = s_ref[...]
        high = value.astype(BF)
        rest = value - high.astype(F32)
        mid = rest.astype(BF)
        low = (rest - mid.astype(F32)).astype(BF)
        row = lax.broadcasted_iota(jnp.int32, (SPARE, columns), 0)
        pick = jnp.where(row == 0, high.astype(F32), jnp.where(row == 1, mid.astype(F32), jnp.where(row == 2, low.astype(F32), 0.0)))
        near_ref[0, :SPARE, :] = pick.astype(BF)

    return pl.pallas_call(
        body,
        out_shape=[
            jax.ShapeDtypeStruct((1, len(stage.near) * LANES + SPARE, columns), BF),
            jax.ShapeDtypeStruct((1, len(stage.far_z) * LANES, columns), BF),
        ],
        in_specs=[SMEM, VMEM, VMEM],
        out_specs=[VMEM, VMEM],
        compiler_params=params(16),
        cost_estimate=cost(1000, 6 * weight.size),
    )(places, weight, scale.reshape(1, columns))


class Stage:
    def __init__(self, name, tiles, unit, axis, head):
        self.name, self.tiles, self.unit, self.axis, self.head = name, tiles, unit, axis, head
        n = len(tiles)
        self.fz, self.fy = max(1, n // 5), n // 2
        back = list(reversed(tiles))
        self.near, self.far_z = tiles[: n - self.fz], back[: self.fz]
        self.near_y, self.far_y = tiles[: n - self.fy], back[: self.fy]

    def runs(self):
        out = []
        unit, head, fz, fy = self.unit, self.head, self.fz, self.fy

        def put(piece, block, count, offset, tiles, with_head=False):
            at = offset
            if with_head:
                at += head
            k = 0
            while k < len(tiles):
                n = 1
                while k + n < len(tiles) and tiles[k + n] == tiles[k] + n:
                    n += 1
                start, size, place = at + k * unit, n * unit, head + tiles[k] * unit
                if with_head and head and k == 0:
                    if tiles[0] == 0:
                        start, size, place = start - head, size + head, place - head
                    else:
                        out.append((piece, block, count, offset, 0, head))
                out.append((piece, block, count, start, place, size))
                k += n

        put(0, 0, 1, 0, self.near, True)
        put(1, 1, 1, 0, self.near, True)
        put(2, 2, 2, 0, self.near, True)
        put(3, 0, 1, 0, self.far_z)
        put(4, 4, 2, 0, self.near_y, True)
        put(5, 6, 2, 0, self.near_y, True)
        put(6, 1, 1, 0, self.far_z)
        put(6, 4, 1, fz * unit, self.far_y)
        put(6, 5, 1, (fz + fy) * unit, self.far_y)
        put(7, 2, 2, 0, self.far_z)
        put(7, 6, 2, fz * unit, self.far_y)
        return out


N_PIECES = 8


def fetches(stage, pieces, scratch, sems, first):
    out = []
    for piece, block, count, start, place, size in stage.runs():
        if stage.axis == 2:
            source = pieces[piece].at[:, :, pl.ds(start, size)]
            target = scratch.at[pl.ds(block, count), :, pl.ds(place, size)]
        else:
            source = pieces[piece].at[:, pl.ds(start, size), :]
            target = scratch.at[pl.ds(block, count), pl.ds(place, size), :]
        out.append(pltpu.make_async_copy(source, target, sems.at[first + len(out)]))
    return out


def norm_rows(rows, gains):
    values = rows.astype(F32)
    factor = lax.rsqrt(jnp.mean(values * values, axis=1, keepdims=True) + EPS)
    return (values * factor * gains).astype(BF)


def local_gain(gain_ref, at, blocks):
    return jnp.concatenate([gain_ref[pl.ds(at[l], 1), :] for l in range(blocks)], axis=1)


def residual_and_norm(rest, weight, terms, gains, new_ref, normed, step, first=0, count=None):
    count = rest.shape[0] if count is None else count

    @pl.loop(0, count // step, unroll=4)
    def _(i):
        here = pl.ds(pl.multiple_of(first + i * step, step), step)
        rows = rest[here, :]
        if terms:
            total = terms[0][here, :].astype(F32) + terms[1][here, :].astype(F32)
            rows = (rows.astype(F32) + weight * total).astype(BF)
            new_ref[here, :] = rows
        normed[here, :] = norm_rows(rows, gains)


def norm_block(rest, weight, terms, gains, new_ref, normed, row, step):
    here = slice(row, row + step)
    rows = rest[here, :]
    total = terms[0][here, :].astype(F32) + terms[1][here, :].astype(F32)
    rows = (rows.astype(F32) + weight * total).astype(BF)
    new_ref[here, :] = rows
    normed[here, :] = norm_rows(rows, gains)


def flat(ref, columns):
    block = ref[:, :, columns]
    return block.reshape(block.shape[0] * block.shape[1], block.shape[2])


def hidden_tile(k, place, lhs, w_up, gs_ref, us_ref, out, here):
    rhs = flat(w_up, slice(2 * k * LANES, (2 * k + 2) * LANES))
    acc = jnp.dot(lhs, rhs, preferred_element_type=F32)
    n = place[k]
    gate = acc[:, :LANES] * gs_ref[pl.ds(n, 1), :]
    up_part = acc[:, LANES:] * us_ref[pl.ds(n, 1), :]
    out[here, k * LANES : (k + 1) * LANES] = (gate / (1.0 + jnp.exp(-gate)) * up_part).astype(BF)


def hidden_units(config, place, normed, w_up, gs_ref, us_ref, out):
    tiles, chunk = config["tiles"], config["chunk"]

    @pl.loop(0, normed.shape[0] // chunk)
    def _(i):
        here = pl.ds(pl.multiple_of(i * chunk, chunk), chunk)
        lhs = normed[here, :]
        for k in range(tiles):
            hidden_tile(k, place, lhs, w_up, gs_ref, us_ref, out, here)


def down_block(left, weight, l):
    acc = jnp.dot(left, weight[l, SPARE:, :], preferred_element_type=F32)
    terms = weight[l, :SPARE, :].astype(F32)
    return (acc * (terms[0:1] + terms[1:2] + terms[2:3])).astype(BF)


def second_pass(config, ids, state, gain, stages, pieces, scales):
    blocks, tiles, chunk, place_of = config["blocks"], config["tiles"], config["chunk"], config["place"]
    count, width = state[0].shape
    columns, units, half = width // blocks, tiles * LANES, width // 2
    n_copies = sum(len(stage.runs()) for stage in stages)
    chunks, step = count // chunk, 16

    def body(*refs):
        at, place, refs = refs[0], refs[1], refs[2:]
        sources, gain_ref, gs_ref, us_ref, refs = refs[:3], refs[3], refs[4], refs[5], refs[6:]
        parts = [refs[N_PIECES * i : N_PIECES * (i + 1)] for i in range(len(stages))]
        refs = refs[N_PIECES * len(stages) :]
        outs, refs = refs[:3], refs[3:]
        w_up, w_down, normed, hidden, new_ref, halves, rests, sems, load_sems, save_sems = refs[:10]
        st = refs[10:]
        rows = [pl.ds(i * chunk, chunk) for i in range(chunks)]
        loads = [
            [pltpu.make_async_copy(a.at[r, :], b.at[r, :], load_sems.at[3 * i + k]) for k, (a, b) in enumerate(zip(sources, st))]
            for i, r in enumerate(rows)
        ]
        copies, at_sem = [], 0
        for stage, part, scratch in zip(stages, parts, (w_up, w_up, w_down)):
            copies.append(fetches(stage, part, scratch, sems, at_sem))
            at_sem += len(copies[-1])
        for group in [loads[0], copies[0], copies[1]] + loads[1:] + [copies[2]]:
            for copy in group:
                copy.start()
        gains = local_gain(gain_ref, at, blocks)
        for copy in loads[0]:
            copy.wait()
        residual_and_norm(st[0], 1.0, st[1:], gains, new_ref, normed, step, 0, chunk)
        saves = []
        for i in range(chunks):
            here = slice(i * chunk, (i + 1) * chunk)
            pending = []
            if i + 1 < chunks:
                pending = list(range((i + 1) * chunk, (i + 2) * chunk, step))
                for copy in loads[i + 1]:
                    copy.wait()
            done = 0
            for s in range(2):
                if i == 0:
                    for copy in copies[s]:
                        copy.wait()
                for k in stages[s].tiles:
                    hidden_tile(k, place, normed[here, :], w_up, gs_ref, us_ref, hidden, here)
                    done += 1
                    share = -(-len(pending) // (tiles - done + 1))
                    for row in pending[:share]:
                        norm_block(st[0], 1.0, st[1:], gains, new_ref, normed, row, step)
                    pending = pending[share:]
            if i == 0:
                for copy in copies[2]:
                    copy.wait()
            left = hidden[here, :]
            for l in range(blocks):
                value = down_block(left, w_down, l)
                j = at[l]
                side = jnp.where(lax.div(j, blocks // 2) == at[blocks], 0, 1)
                there = pl.ds(pl.multiple_of(lax.rem(j, blocks // 2) * columns, columns), columns)
                halves[side, here, there] = value
                rests[side, here, there] = new_ref[here, l * columns : (l + 1) * columns]
            results = ((halves.at[1], outs[1]), (halves.at[0], outs[0]), (rests.at[0], outs[2]))
            for k, (a, b) in enumerate(results):
                saves.append(pltpu.make_async_copy(a.at[rows[i], :], b.at[rows[i], :], save_sems.at[3 * i + k]))
                saves[-1].start()
        for copy in saves:
            copy.wait()

    return pl.pallas_call(
        body,
        out_shape=[jax.ShapeDtypeStruct((count, half), BF)] * 3,
        in_specs=[SMEM, SMEM] + [ANY] * 3 + [VMEM] * 3 + [HBM] * (N_PIECES * len(stages)),
        out_specs=[ANY] * 3,
        scratch_shapes=[
            pltpu.VMEM((blocks, columns, 2 * units), BF),
            pltpu.VMEM((blocks, SPARE + units, columns), BF),
            pltpu.VMEM((count, width), BF),
            pltpu.VMEM((count, units), BF),
            pltpu.VMEM((count, width), BF),
            pltpu.VMEM((2, count, half), BF),
            pltpu.VMEM((2, count, half), BF),
            pltpu.SemaphoreType.DMA((n_copies,)),
            pltpu.SemaphoreType.DMA((3 * chunks,)),
            pltpu.SemaphoreType.DMA((3 * chunks,)),
        ]
        + [pltpu.VMEM((count, width), BF)] * 3,
        compiler_params=params(55),
        cost_estimate=cost(6 * count * width * units, 2 * 3 * width * units),
    )(
        ids,
        place_of,
        *state,
        gain.reshape(blocks, columns),
        scales[0].reshape(tiles, LANES),
        scales[1].reshape(tiles, LANES),
        *[p for group in pieces for p in group],
    )


def first_hidden(config, ids, state, gain, stages, pieces, scales):
    blocks, tiles = config["blocks"], config["tiles"]
    count, width = state.shape
    columns, units = width // blocks, tiles * LANES
    n_copies = sum(len(stage.runs()) for stage in stages)

    def body(at, place, source, gain_ref, gs_ref, us_ref, *refs):
        parts = [refs[N_PIECES * i : N_PIECES * (i + 1)] for i in range(len(stages))]
        out, w_up, normed, sems, st = refs[N_PIECES * len(stages) :]
        load = pltpu.make_async_copy(source, st, sems.at[n_copies])
        up = []
        for stage, part in zip(stages, parts):
            up += fetches(stage, part, w_up, sems, len(up))
        for copy in [load] + up:
            copy.start()
        gains = local_gain(gain_ref, at, blocks)
        load.wait()
        residual_and_norm(st, 0.5, (), gains, None, normed, 16)
        for copy in up:
            copy.wait()
        hidden_units(config, place, normed, w_up, gs_ref, us_ref, out)

    return pl.pallas_call(
        body,
        out_shape=jax.ShapeDtypeStruct((count, units), BF),
        in_specs=[SMEM, SMEM, HBM] + [VMEM] * 3 + [HBM] * (N_PIECES * len(stages)),
        out_specs=VMEM,
        scratch_shapes=[
            pltpu.VMEM((blocks, columns, 2 * units), BF),
            pltpu.VMEM((count, width), BF),
            pltpu.SemaphoreType.DMA((n_copies + 1,)),
            pltpu.VMEM((count, width), BF),
        ],
        compiler_params=params(24),
        cost_estimate=cost(4 * count * width * units, 2 * 2 * width * units),
    )(
        ids,
        config["place"],
        state,
        gain.reshape(blocks, columns),
        scales[0].reshape(tiles, LANES),
        scales[1].reshape(tiles, LANES),
        *[p for group in pieces for p in group],
    )


def first_down(config, hidden, stage, pieces):
    blocks, chunk, width = config["blocks"], config["chunk"], config["width"]
    count, units = hidden.shape
    columns = width // blocks
    n_copies = len(stage.runs())

    def body(left_ref, *refs):
        out, w_down, sems = refs[N_PIECES:]
        copies = fetches(stage, refs[:N_PIECES], w_down, sems, 0)
        for copy in copies:
            copy.start()
        for copy in copies:
            copy.wait()

        @pl.loop(0, count // chunk)
        def _(i):
            here = pl.ds(pl.multiple_of(i * chunk, chunk), chunk)
            left = left_ref[here, :]
            for l in range(blocks):
                out[here, l * columns : (l + 1) * columns] = down_block(left, w_down, l)

    return pl.pallas_call(
        body,
        out_shape=jax.ShapeDtypeStruct((count, width), BF),
        in_specs=[VMEM] + [HBM] * N_PIECES,
        out_specs=VMEM,
        scratch_shapes=[pltpu.VMEM((blocks, SPARE + units, columns), BF), pltpu.SemaphoreType.DMA((n_copies,))],
        compiler_params=params(16),
        cost_estimate=cost(2 * count * width * units, 2 * width * units),
    )(hidden, *pieces)


def gelu(a):
    return 0.5 * a * (1.0 + jnp.tanh(0.7978845608028654 * (a + 0.044715 * a * a * a)))


def mixer_in(config, ids, state, gain, stage, pieces, scales):
    blocks, tiles, chunk = config["blocks"], config["tiles"], config["chunk"]
    count, width = state[0].shape
    columns = width // blocks
    n_copies = len(stage.runs())
    chunks, step = count // chunk, 16

    def body(*refs):
        at, place, refs = refs[0], refs[1], refs[2:]
        sources, gain_ref, us_ref, vs_ref = refs[:3], refs[3], refs[4], refs[5]
        parts, refs = refs[6 : 6 + N_PIECES], refs[6 + N_PIECES :]
        new_out, u_out, v_out, sum_out, w, normed, sems, load_sems, *st = refs
        rows = [pl.ds(i * chunk, chunk) for i in range(chunks)]
        loads = [
            [pltpu.make_async_copy(a.at[r, :], b.at[r, :], load_sems.at[3 * i + k]) for k, (a, b) in enumerate(zip(sources, st))]
            for i, r in enumerate(rows)
        ]
        copies = fetches(stage, parts, w, sems, 0)
        for group in [loads[0], copies] + loads[1:]:
            for copy in group:
                copy.start()
        gains = local_gain(gain_ref, at, blocks)
        for copy in loads[0]:
            copy.wait()
        residual_and_norm(st[0], 0.5, st[1:], gains, new_out, normed, step, 0, chunk)
        for copy in copies:
            copy.wait()
        for i in range(chunks):
            here = slice(i * chunk, (i + 1) * chunk)
            pending = []
            if i + 1 < chunks:
                pending = list(range((i + 1) * chunk, (i + 2) * chunk, step))
                for copy in loads[i + 1]:
                    copy.wait()
            lhs = normed[here, :]
            plain = jnp.zeros((chunk, LANES), F32)
            square = jnp.zeros((chunk, LANES), F32)
            for k in range(tiles):
                rhs = flat(w, slice(2 * k * LANES, (2 * k + 2) * LANES))
                acc = jnp.dot(lhs, rhs, preferred_element_type=F32)
                n = place[k]
                block = slice(k * LANES, (k + 1) * LANES)
                u_out[here, block] = gelu(acc[:, :LANES] * us_ref[pl.ds(n, 1), :])
                v_act = gelu(acc[:, LANES:] * vs_ref[pl.ds(n, 1), :])
                v_out[here, block] = v_act
                plain += v_act
                square += v_act * v_act
                share = -(-len(pending) // (tiles - k))
                for row in pending[:share]:
                    norm_block(st[0], 0.5, st[1:], gains, new_out, normed, row, step)
                pending = pending[share:]
            index = lax.broadcasted_iota(jnp.int32, (chunk, LANES), 1)
            sum_out[here, :] = jnp.where(
                index == 0, jnp.sum(plain, axis=1, keepdims=True), jnp.sum(square, axis=1, keepdims=True)
            )

    return pl.pallas_call(
        body,
        out_shape=[
            jax.ShapeDtypeStruct((count, width), BF),
            jax.ShapeDtypeStruct((count, tiles * LANES), F32),
            jax.ShapeDtypeStruct((count, tiles * LANES), F32),
            jax.ShapeDtypeStruct((count, LANES), F32),
        ],
        in_specs=[SMEM, SMEM] + [ANY] * 3 + [VMEM] * 3 + [HBM] * N_PIECES,
        out_specs=[VMEM] * 4,
        scratch_shapes=[
            pltpu.VMEM((blocks, columns, 2 * tiles * LANES), BF),
            pltpu.VMEM((count, width), BF),
            pltpu.SemaphoreType.DMA((n_copies,)),
            pltpu.SemaphoreType.DMA((3 * chunks,)),
        ]
        + [pltpu.VMEM((count, width), BF)] * 3,
        compiler_params=params(48),
        cost_estimate=cost(4 * count * width * tiles * LANES, 4 * width * tiles * LANES),
    )(
        ids,
        config["place"],
        *state,
        gain.reshape(blocks, columns),
        scales[0].reshape(tiles, LANES),
        scales[1].reshape(tiles, LANES),
        *pieces,
    )


def mixer_out(config, u_act, v_act, sums, other, layer, spatial_weight, spatial_bias, stage, pieces):
    blocks, tiles, chunk, width = config["blocks"], config["tiles"], config["chunk"], config["width"]
    count, channels = u_act.shape
    columns = width // blocks
    span = spatial_weight.shape[1]
    n_copies = len(stage.runs())
    share = 0.5 / channels

    def body(*refs):
        place, u_ref, v_ref, s_ref, o_ref, gain_ref, bias_ref, w_ref, b_ref = refs[:9]
        parts, refs = refs[9 : 9 + N_PIECES], refs[9 + N_PIECES :]
        out, w_out, mixed, sems = refs
        copies = fetches(stage, parts, w_out, sems, 0)
        for copy in copies:
            copy.start()
        total = s_ref[...] + o_ref[...]
        mean = total[:, 0:1] * share
        var = total[:, 1:2] * share - mean * mean
        factor = lax.rsqrt(var + EPS)
        keep = lax.broadcasted_iota(jnp.int32, (span, span), 0) >= lax.broadcasted_iota(jnp.int32, (span, span), 1)
        for t in range(tiles):
            n = place[t]
            block = slice(t * LANES, (t + 1) * LANES)
            v_normed = ((v_ref[:, block] - mean) * factor * gain_ref[pl.ds(n, 1), :] + bias_ref[pl.ds(n, 1), :]).astype(BF)
            side = jnp.concatenate([v_normed[m * span : (m + 1) * span] for m in range(count // span)], axis=1)
            w = jnp.where(keep, w_ref[n].astype(F32), 0.0).astype(BF)
            turned = jnp.dot(w, side, preferred_element_type=F32)
            shift = b_ref[n]
            for m in range(count // span):
                here = slice(m * span, (m + 1) * span)
                spatial = turned[:, m * LANES : (m + 1) * LANES] + shift
                mixed[here, block] = (u_ref[here, block] * spatial).astype(BF)
        for copy in copies:
            copy.wait()

        @pl.loop(0, count // chunk)
        def _(i):
            here = pl.ds(pl.multiple_of(i * chunk, chunk), chunk)
            left = mixed[here, :]
            for l in range(blocks):
                out[here, l * columns : (l + 1) * columns] = down_block(left, w_out, l)

    return pl.pallas_call(
        body,
        out_shape=jax.ShapeDtypeStruct((count, width), BF),
        in_specs=[SMEM] + [VMEM] * 8 + [HBM] * N_PIECES,
        out_specs=VMEM,
        scratch_shapes=[
            pltpu.VMEM((blocks, SPARE + channels, columns), BF),
            pltpu.VMEM((count, channels), BF),
            pltpu.SemaphoreType.DMA((n_copies,)),
        ],
        compiler_params=params(50),
        cost_estimate=cost(2 * count * width * channels, 2 * width * channels),
    )(
        config["place"],
        u_act,
        v_act,
        sums,
        other,
        layer[0].reshape(tiles, LANES),
        layer[1].reshape(tiles, LANES),
        spatial_weight,
        jnp.broadcast_to(spatial_bias[:, :, None], (tiles, span, LANES)),
        *pieces,
    )


SWAP = [(0, 1), (1, 0)]
NZ, NY = 4, 2


def join(body, shapes, flag, *values):
    return pl.pallas_call(
        body,
        out_shape=[jax.ShapeDtypeStruct(shape, BF) for shape in shapes],
        in_specs=[SMEM] + [VMEM] * len(values),
        out_specs=[VMEM] * len(shapes),
        compiler_params=params(12),
        cost_estimate=cost(1000000, 4 * sum(v.size for v in values)),
    )(flag, *values)


def gather(stage, near, far, outer):
    at = lambda z, y: z * NY + y
    pairs = lambda hops: [(at(a, y), at(b, y)) for a, b in hops for y in range(NY)]
    across = [(at(z, y), at(z, 1 - y)) for z in range(NZ) for y in range(NY)]
    axis = stage.axis
    unit, head = stage.unit, stage.head
    all_z, all_y = head + len(stage.near) * unit, head + len(stage.near_y) * unit
    fz, fy = stage.fz * unit, stage.fy * unit

    def shape(blocks, size):
        out = [blocks, near.shape[1], near.shape[2]]
        out[axis] = size
        return tuple(out)

    def part(ref, block, start, size):
        return ref.at[block, pl.ds(start, size), :] if axis == 1 else ref.at[block, :, pl.ds(start, size)]

    def put(to, block, start, source, at, begin, size):
        part(to, block, start, size)[...] = part(source, at, begin, size)[...]

    def join_e(_, near_ref, e_ref, m_ref, y_ref):
        for k, ref in enumerate((near_ref, e_ref)):
            put(m_ref, k, 0, ref, 0, 0, all_z)
            put(y_ref, k, 0, ref, 0, 0, all_y)

    def join_p(_, e_ref, y_ref, p_ref):
        put(p_ref, 0, 0, e_ref, 0, head, fz)
        for k in range(2):
            put(p_ref, 0, fz + k * fy, y_ref, k, head, fy)

    def join_g(is_outer, g_ref, m_ref, two_ref, r_ref):
        def take(ref):
            for k in range(2):
                put(two_ref, k, 0, ref, k, 0, all_z)
                put(r_ref, k, 0, ref, k, 0, all_y)

        pl.when(is_outer[0] == 1)(lambda: take(g_ref))
        pl.when(is_outer[0] == 0)(lambda: take(m_ref))

    def join_q(_, two_ref, r_ref, q_ref):
        for k in range(2):
            put(q_ref, k, 0, two_ref, k, head, fz)
            put(q_ref, k, fz, r_ref, k, head, fy)

    e = lax.ppermute(near, "fs", pairs([(0, 1), (1, 0), (2, 3), (3, 2)]))
    m, y = join(join_e, [shape(2, all_z), shape(2, all_y)], outer, near, e)
    m = lax.ppermute(m, "fs", pairs([(1, 2), (2, 1)]))
    y = lax.ppermute(y, "fs", across)
    g = lax.ppermute(m, "fs", pairs([(1, 0), (2, 3)]))
    (p,) = join(join_p, [shape(1, fz + 2 * fy)], outer, e, y)
    p = lax.ppermute(p, "rep", SWAP)
    two, r = join(join_g, [shape(2, all_z), shape(2, all_y)], outer, g, m)
    r = lax.ppermute(r, "fs", across)
    (q,) = join(join_q, [shape(2, fz + fy)], outer, two, r)
    q = lax.ppermute(q, "rep", SWAP)
    return [near, e, two, far, y, r, p, q]


def fast(*args):
    (tokens, norm_first, norm_mix, norm_second, gate_weight, up_weight, down_weight, gate_scale, up_scale, down_scale,
     u_weight, v_weight, u_scale, v_scale, ln_gain, ln_bias, spatial_weight, spatial_bias, out_weight, out_scale) = args
    count, half = tokens.shape
    width = 2 * half
    blocks = NZ * NY
    columns = width // blocks
    rep, tp, fs = lax.axis_index("rep"), lax.axis_index("tp"), lax.axis_index("fs")
    z, y = fs // NY, fs % NY
    outer = jnp.logical_or(z == 0, z == NZ - 1).astype(jnp.int32).reshape(1)
    low = z < 2
    layers = (z, z + 1 - 2 * (z % 2), jnp.where(low, 2, 1), jnp.where(low, 3, 0))
    ids = jnp.stack([layer * NY + row for row in (y, 1 - y) for layer in layers] + [tp]).astype(jnp.int32)
    ff_tiles, bw_tiles = gate_weight.shape[1] // LANES, u_weight.shape[1] // LANES

    def places(tiles):
        index = jnp.arange(tiles, dtype=jnp.int32)
        return jnp.where(rep == 0, index, tiles - 1 - index)

    ff_place, bw_place = places(ff_tiles), places(bw_tiles)
    rim = ff_tiles // 5
    every = list(range(ff_tiles))
    outside = every[:rim] + [ff_tiles // 2] * (ff_tiles % 2) + every[ff_tiles - rim :]
    inside = [k for k in every if k not in outside]
    g1, g2 = Stage("g1", outside, 2 * LANES, 2, 0), Stage("g2", inside, 2 * LANES, 2, 0)
    dn = Stage("dn", every, LANES, 1, SPARE)
    uv = Stage("uv", list(range(bw_tiles)), 2 * LANES, 2, 0)
    ou = Stage("ou", list(range(bw_tiles)), LANES, 1, SPARE)
    own = {}
    own["g1"], own["g2"] = pack_pairs(gate_weight, up_weight, ff_place, [g1, g2])
    own["dn"] = pack_rows(down_weight, down_scale, ff_place, dn)
    (own["uv"],) = pack_pairs(u_weight, v_weight, bw_place, [uv])
    own["ou"] = pack_rows(out_weight, out_scale, bw_place, ou)
    peer = lax.ppermute(tokens, "tp", SWAP)
    pieces = {s.name: gather(s, *own[s.name], outer) for s in (g1, g2, dn, uv, ou)}
    full = jnp.where(tp == 0, jnp.concatenate([tokens, peer], axis=1), jnp.concatenate([peer, tokens], axis=1))
    start = jnp.concatenate([lax.dynamic_slice_in_dim(full, ids[l] * columns, columns, axis=1) for l in range(blocks)], axis=1)
    chunk = count // 2
    ff = {"blocks": blocks, "tiles": ff_tiles, "chunk": chunk, "place": ff_place, "width": width}
    mix = {"blocks": blocks, "tiles": bw_tiles, "chunk": chunk, "place": bw_place, "width": width}
    ff_stages, ff_pieces = (g1, g2, dn), [pieces["g1"], pieces["g2"], pieces["dn"]]
    hidden = first_hidden(ff, ids, start, norm_first, ff_stages[:2], ff_pieces[:2], (gate_scale, up_scale))
    first = first_down(ff, hidden, dn, pieces["dn"])
    first_in = lax.ppermute(first, "tp", SWAP)
    middle, u_act, v_act, sums = mixer_in(mix, ids, (start, first, first_in), norm_mix, uv, pieces["uv"], (u_scale, v_scale))
    sums_in = lax.ppermute(sums, "tp", SWAP)
    mixed = mixer_out(mix, u_act, v_act, sums, sums_in, (ln_gain, ln_bias), spatial_weight, spatial_bias, ou, pieces["ou"])
    mixed_in = lax.ppermute(mixed, "tp", SWAP)
    own_last, send, rest = second_pass(
        ff, ids, (middle, mixed, mixed_in), norm_second, ff_stages, ff_pieces, (gate_scale, up_scale))
    got = lax.ppermute(send, "tp", SWAP)
    return (rest.astype(F32) + 0.5 * (own_last.astype(F32) + got.astype(F32))).astype(BF)


def plain(*args):
    (tokens, norm_first, norm_mix, norm_second, gate_weight, up_weight, down_weight, gate_scale, up_scale, down_scale,
     u_weight, v_weight, u_scale, v_scale, ln_gain, ln_bias, spatial_weight, spatial_bias, out_weight, out_scale) = args
    gather = lambda v, axis: lax.all_gather(v, "fs", axis=axis, tiled=True)
    count, n_tp = tokens.shape[0], lax.axis_size("tp")
    span = spatial_weight.shape[1]

    def full_norm(rows, gain):
        values = lax.all_gather(rows, "tp", axis=1, tiled=True).astype(F32)
        factor = lax.rsqrt(jnp.mean(values * values, axis=1, keepdims=True) + EPS)
        return (values * factor * gain).astype(BF)

    def spread_sum(term):
        return lax.psum_scatter(term.astype(BF), "tp", scatter_dimension=1, tiled=True).astype(F32)

    def dot(left, right):
        return jnp.dot(left, right, preferred_element_type=F32)

    gate_all, up_all, down_all = gather(gate_weight.astype(BF), 0), gather(up_weight.astype(BF), 0), gather(down_weight.astype(BF), 1)
    down_scales, out_scales = gather(down_scale, 0), gather(out_scale, 0)

    def feed(rows, gain):
        normed = full_norm(rows, gain)
        hidden = (jax.nn.silu(dot(normed, gate_all) * gate_scale) * (dot(normed, up_all) * up_scale)).astype(BF)
        return spread_sum(dot(hidden, down_all) * down_scales)

    middle = (tokens.astype(F32) + 0.5 * feed(tokens, norm_first)).astype(BF)
    normed = full_norm(middle, norm_mix)
    u_pre = dot(normed, gather(u_weight.astype(BF), 0)) * u_scale
    v_act = gelu(dot(normed, gather(v_weight.astype(BF), 0)) * v_scale)
    sums = lax.psum((jnp.sum(v_act, axis=1), jnp.sum(v_act * v_act, axis=1)), "tp")
    channels = v_act.shape[1]
    v_mean = (sums[0] / (n_tp * channels))[:, None]
    v_var = (sums[1] / (n_tp * channels))[:, None] - v_mean * v_mean
    v_normed = ((v_act - v_mean) * lax.rsqrt(v_var + EPS) * ln_gain + ln_bias).astype(BF)
    groups = spatial_weight.shape[0]
    tiles = v_normed.reshape(count // span, span, groups, channels // groups)
    lower = jnp.tril(jnp.ones((span, span), jnp.bool_))
    masked = jnp.where(lower[None], spatial_weight, jnp.zeros_like(spatial_weight))
    spatial = jnp.einsum("gts,nsgc->ntgc", masked, tiles, preferred_element_type=F32) + spatial_bias.T[None, :, :, None]
    mixed = (gelu(u_pre) * spatial.reshape(count, channels)).astype(BF)
    second = (middle.astype(F32) + spread_sum(dot(mixed, gather(out_weight.astype(BF), 1)) * out_scales)).astype(BF)
    return (second.astype(F32) + 0.5 * feed(second, norm_second)).astype(BF)


def solution(mesh):
    tokens = P(("rep", "fs"), "tp")
    rows, columns = P("fs", "tp"), P("tp", "fs")
    tp, fs, whole = P("tp"), P("fs"), P()
    placed = (
        tokens, whole, whole, whole, rows, rows, columns, tp, tp, fs, rows, rows, tp, tp, tp, tp,
        P("tp", None, None), P("tp", None), columns, fs,
    )

    def on_device(*args):
        block = args[4].shape[0]
        tidy = block % (2 * LANES) == 0 and args[4].shape[1] % LANES == 0 and args[10].shape[1] % LANES == 0
        if tidy and mesh.shape["fs"] == NZ * NY and mesh.shape["rep"] == 2 and mesh.shape["tp"] == 2:
            return fast(*args)
        return plain(*args)

    return jax.shard_map(on_device, mesh=mesh, in_specs=placed, out_specs=tokens, check_vma=False)
```
